32 devices in a mesh: sp: 8 (over z, y), tp: 4 (over x, core).
Axes of the slice: x: 2, y: 2, z: 4, core: 2. Of those that a mesh axis runs over, the one named last changes fastest.
Arguments:
- tokens: bfloat16 [2048, 4096], P('sp'), may hold values from -64 to 64
- norm_gain: float32 [4096], replicated, may hold values from 0.1 to 1.9
- w_query: bfloat16 [4096, 2048], P('sp', 'tp'), may hold values from -1.09375 to 1.09375
- w_key: bfloat16 [4096, 512], P('sp', 'tp'), may hold values from -0.09375 to 0.09375
- w_value: bfloat16 [4096, 512], P('sp', 'tp'), may hold values from -0.09375 to 0.09375
- w_glu: bfloat16 [4096, 2048], P('sp', 'tp'), may hold values from -0.09375 to 0.09375
- w_gate: bfloat16 [4096, 2048], P('sp', 'tp'), may hold values from -0.09375 to 0.09375
- sink_logit: float32 [32], P('tp'), may hold values from 2 to 6
- conv_taps: bfloat16 [31, 2048], P(None, 'tp'), may hold values from -12.9315817 to 12.9315817
- conv_gain: float32 [2048], P('tp'), may hold values from 0.1 to 1.9
- out_attn: bfloat16 [2048, 4096], P('sp', 'tp'), may hold values from -0.5 to 0.5
- out_conv: bfloat16 [2048, 4096], P('sp', 'tp'), may hold values from -0.125 to 0.125
Outputs:
- mixed: bfloat16 [2048, 4096], P('sp', 'tp')
The draws below stay inside these ranges and needn't reach their ends.
All inputs are finite; a program needn't handle non-finite values.
Results may differ from the reference program's by a relative error of at most 0.008.
The reference program's roundings to bfloat16 on the way count: a program that leaves them out, or rounds other values in their place, can miss the bound.
Values may be sent and summed in bfloat16 or wider, within the bound.
A program may use at most 64 MiB of HBM per device.

```python
import math
import jax
import jax.numpy as jnp
from jax import lax

D = 4096
HEADS = 32
HEAD = 64
KV = 8
CONV = 2048
KSIZE = 31
WINDOW = 128
TOKENS = 2048


def draw_tokens(key, part):
    subkeys = jax.random.split(key, 3)
    row_scale = jnp.exp(jax.random.uniform(subkeys[0], (TOKENS, 1), jnp.float32, 0.0, math.log(4.0)))
    col_scale = jnp.exp(jax.random.uniform(subkeys[1], (1, D), jnp.float32, 0.0, math.log(4.0)))
    raw_draw = jnp.clip(jax.random.normal(subkeys[2], (TOKENS, D), jnp.float32), -4.0, 4.0)
    return (raw_draw * row_scale * col_scale).astype(jnp.bfloat16)


def draw_w_query(key, part):
    spread = D ** (-0.5)
    raw_draw = jnp.clip(jax.random.normal(key, (D, HEADS * HEAD), jnp.float32), -4.0, 4.0)
    return (raw_draw * spread).astype(jnp.bfloat16)


def draw_conv_taps(key, part):
    subkeys = jax.random.split(key, 2)
    channel = jnp.arange(CONV, dtype=jnp.float32)[None, :] / CONV
    jitter = jnp.exp(jax.random.uniform(subkeys[0], (1, CONV), jnp.float32, math.log(0.7), math.log(1.4)))
    rising = 10.0 ** channel
    raw_draw = jnp.clip(jax.random.normal(subkeys[1], (KSIZE, CONV), jnp.float32), -4.0, 4.0)
    return (raw_draw * rising * jitter * KSIZE ** (-0.5)).astype(jnp.bfloat16)


def steps_of(rng, shape, shards, smallest, largest):
    level = 1.0
    for dim, blocks in shards:
        heights = jax.random.uniform(jax.random.fold_in(jax.random.fold_in(rng, 6), dim), (blocks,), jnp.float32, smallest / len(shards), largest / len(shards))
        level = level * jnp.repeat(jnp.exp(heights), shape[dim] // blocks).reshape((-1,) + (1,) * (len(shape) - 1 - dim))
    return level


def scatter_about(stream_key, shape, width, limit, pieces=(), held_as=jnp.bfloat16):
    gain = steps_of(stream_key, shape, pieces, -0.22, 0.18) if pieces else 1.0
    array = jax.random.normal(stream_key, shape, jnp.float32) * width * gain
    return jnp.minimum(jnp.maximum(array, -limit), limit).astype(held_as)


def setup_inputs(seed: int = 0) -> dict:
    key_of = jax.random.split(jax.random.key(seed), 13)
    tokens = draw_tokens(jax.random.fold_in(key_of[12], 71), 0)
    norm_gain = jnp.clip(1.0 + 0.18 * jax.random.normal(key_of[1], (D,), jnp.float32), 0.1, 1.9)
    w_query = draw_w_query(jax.random.fold_in(key_of[12], 71), 0)
    w_key = scatter_about(key_of[3], (D, KV * HEAD), D ** -0.5, 0.09375, ((0, 8), (1, 4)))
    w_value = scatter_about(key_of[4], (D, KV * HEAD), D ** -0.5, 0.09375, ((0, 8), (1, 4)))
    w_glu = scatter_about(key_of[5], (D, CONV), D ** -0.5, 0.09375, ((0, 8), (1, 4)))
    w_gate = scatter_about(key_of[6], (D, CONV), D ** -0.5, 0.09375, ((0, 8), (1, 4)))
    sink_logit = jnp.clip(2.0 + 4.0 * jax.random.uniform(key_of[7], (HEADS,), jnp.float32) ** steps_of(key_of[7], (HEADS,), ((0, 4),), -0.2, 0.2), 2.0, 6.0)
    conv_taps = draw_conv_taps(jax.random.fold_in(key_of[12], 71), 0)
    conv_gain = jnp.clip(1.0 + 0.18 * jax.random.normal(key_of[9], (CONV,), jnp.float32), 0.1, 1.9)
    out_attn = scatter_about(key_of[10], (HEADS * HEAD, D), (HEADS * HEAD // 16) ** -0.5, 0.5, ((0, 8), (1, 4)))
    out_conv = scatter_about(key_of[11], (CONV, D), CONV ** -0.5, 0.125, ((0, 8), (1, 4)))
    return {"tokens": tokens, "norm_gain": norm_gain, "w_query": w_query, "w_key": w_key, "w_value": w_value, "w_glu": w_glu, "w_gate": w_gate, "sink_logit": sink_logit, "conv_taps": conv_taps, "conv_gain": conv_gain, "out_attn": out_attn, "out_conv": out_conv}


def rotate_heads(values, positions):
    half_width = values.shape[-1] // 2
    frequency = 10000.0 ** (-jnp.arange(half_width, dtype=jnp.float32) * 2.0 / values.shape[-1])
    angles = positions.astype(jnp.float32)[:, None] * frequency[None, :]
    cosine = jnp.cos(angles)[:, None, :]
    sine_part = jnp.sin(angles)[:, None, :]
    first_half = values[..., :half_width]
    second_half = values[..., half_width:]
    return jnp.concatenate([first_half * cosine - second_half * sine_part, second_half * cosine + first_half * sine_part], axis=-1)

def window_attention(operands):
    queries, keys_rot, values_bf, sinks = operands
    total_rows, group_size, head_dimension = queries.shape
    block_count = total_rows // WINDOW
    query_block_rows = queries.reshape(block_count, WINDOW, group_size, head_dimension).astype(jnp.float32)
    key_blocks = keys_rot.reshape(block_count, WINDOW, head_dimension).astype(jnp.float32)
    value_blocks = values_bf.reshape(block_count, WINDOW, head_dimension).astype(jnp.float32)
    empty_block = jnp.zeros((1, WINDOW, head_dimension), jnp.float32)
    key_pair_rows = jnp.concatenate([jnp.concatenate([empty_block, key_blocks[:-1]], axis=0), key_blocks], axis=1)
    value_pair_rows = jnp.concatenate([jnp.concatenate([empty_block, value_blocks[:-1]], axis=0), value_blocks], axis=1)
    score_matrix = jnp.einsum('schn,svn->shcv', query_block_rows, key_pair_rows) * (1.0 / math.sqrt(head_dimension))
    block_ids = jnp.arange(block_count, dtype=jnp.int32)[:, None, None]
    query_pos = block_ids * WINDOW + jnp.arange(WINDOW, dtype=jnp.int32)[None, :, None]
    key_pos = (block_ids - 1) * WINDOW + jnp.arange(2 * WINDOW, dtype=jnp.int32)[None, None, :]
    distance = query_pos - key_pos
    allowed = (distance >= 0) & (distance < WINDOW) & (key_pos >= 0)
    score_matrix = jnp.where(allowed[:, None], score_matrix, -1e+30)
    sink_col = sinks.astype(jnp.float32)[None, :, None, None]
    highest = jnp.maximum(lax.optimization_barrier(jnp.max(score_matrix, axis=-1, keepdims=True)), sink_col)
    weights_exp = jnp.exp(score_matrix - highest)
    denom_total = lax.optimization_barrier(jnp.sum(weights_exp, axis=-1, keepdims=True)) + jnp.exp(sink_col - highest)
    weights_bfloat_half = (weights_exp / denom_total).astype(jnp.bfloat16)
    attended_values = jnp.einsum('jxcp,jpi->jcxi', weights_bfloat_half.astype(jnp.float32), value_pair_rows).astype(jnp.bfloat16)
    return attended_values.reshape(total_rows, group_size, head_dimension)

def reference(tokens, norm_gain, w_query, w_key, w_value, w_glu, w_gate, sink_logit, conv_taps, conv_gain, out_attn, out_conv):
    total_rows = tokens.shape[0]
    tokens_f = tokens.astype(jnp.float32)
    normed = (tokens_f * lax.rsqrt(lax.optimization_barrier(jnp.mean(tokens_f * tokens_f, axis=1, keepdims=True)) + 1e-06) * norm_gain.astype(jnp.float32)).astype(jnp.bfloat16)
    positions = jnp.arange(total_rows, dtype=jnp.int32)
    queries = rotate_heads(jnp.dot(normed, w_query, preferred_element_type=jnp.float32).reshape(total_rows, HEADS, HEAD), positions).astype(jnp.bfloat16)
    keys_rot = rotate_heads(jnp.dot(normed, w_key, preferred_element_type=jnp.float32).reshape(total_rows, KV, HEAD), positions).astype(jnp.bfloat16)
    values_bf = jnp.dot(normed, w_value, preferred_element_type=jnp.float32).astype(jnp.bfloat16).reshape(total_rows, KV, HEAD)
    group_size = HEADS // KV
    query_heads = jnp.transpose(queries.reshape(total_rows, KV, group_size, HEAD), (1, 0, 2, 3))
    key_heads = jnp.transpose(keys_rot, (1, 0, 2))
    value_heads = jnp.transpose(values_bf, (1, 0, 2))
    sink_heads = sink_logit.reshape(KV, group_size)
    attended_values = lax.map(window_attention, (query_heads, key_heads, value_heads, sink_heads))
    attended_values = jnp.transpose(attended_values, (1, 0, 2, 3)).reshape(total_rows, HEADS * HEAD)
    glu_part = jnp.dot(normed, w_glu, preferred_element_type=jnp.float32)
    gate_part = jnp.dot(normed, w_gate, preferred_element_type=jnp.float32)
    gated = (glu_part * jax.nn.sigmoid(gate_part)).astype(jnp.bfloat16)
    extended = jnp.concatenate([jnp.zeros((KSIZE - 1, CONV), jnp.float32), gated.astype(jnp.float32)], axis=0)
    filtered = lax.conv_general_dilated(extended[None], conv_taps.astype(jnp.float32)[:, None, :], (1,), 'VALID', dimension_numbers=('NWC', 'WIO', 'NWC'), feature_group_count=CONV, precision=lax.Precision.HIGHEST)[0]
    mean_value = lax.optimization_barrier(jnp.sum(filtered, axis=1)) / CONV
    variance = lax.optimization_barrier(jnp.sum(filtered * filtered, axis=1)) / CONV - mean_value * mean_value
    scaled = (filtered - mean_value[:, None]) * lax.rsqrt(variance + 1e-05)[:, None] * conv_gain.astype(jnp.float32)
    conv_out = jax.nn.silu(scaled).astype(jnp.bfloat16)
    mixed = jnp.dot(attended_values, out_attn, preferred_element_type=jnp.float32) + jnp.dot(conv_out, out_conv, preferred_element_type=jnp.float32)
    return mixed.astype(jnp.bfloat16)
```

```python
import functools
import math

import jax
import jax.numpy as jnp
from jax import lax
from jax.experimental import pallas as pl
from jax.experimental.pallas import tpu as pltpu
from jax.sharding import PartitionSpec as P

HEADS = 32
HEAD = 64
KV = 8
CONV = 2048
KSIZE = 31
WINDOW = 128


def passed_along(block, axis, distance):
    devices = range(lax.axis_size(axis))
    route = [(i - distance, i) for i in devices if i - distance in devices]
    return lax.ppermute(block, axis, route)


def rotate_heads(values, positions):
    half_width = values.shape[-1] // 2
    frequency = 10000.0 ** (-jnp.arange(half_width, dtype=jnp.float32) * 2.0 / values.shape[-1])
    angles = positions.astype(jnp.float32)[:, None] * frequency[None, :]
    cosine = jnp.cos(angles)[:, None, :]
    sine_part = jnp.sin(angles)[:, None, :]
    first_half = values[..., :half_width]
    second_half = values[..., half_width:]
    return jnp.concatenate(
        [
            first_half * cosine - second_half * sine_part,
            second_half * cosine + first_half * sine_part,
        ],
        axis=-1,
    )


def ring_gather_kernel(n, count, *refs):
    shards, wholes = refs[:count], refs[count : 2 * count]
    bounce = refs[2 * count : 3 * count]
    in_sem, out_sem, send_sem, recv_sem = refs[3 * count :]
    me = lax.axis_index("sp")
    half = n // 2
    odd = lax.rem(me, 2)
    place = (1 - odd) * lax.div(me, 2) + odd * (n - 1 - lax.div(me, 2))

    def device_at(position):
        spot = lax.rem(position + 2 * n, n)
        back = lax.div(spot, half)
        return (1 - back) * 2 * spot + back * (2 * (n - 1 - spot) + 1)

    ahead, behind = device_at(place + 1), device_at(place - 1)
    barrier = pltpu.get_barrier_semaphore()
    for neighbour in (ahead, behind):
        pl.semaphore_signal(
            barrier, inc=1, device_id={"sp": neighbour}, device_id_type=pl.DeviceIdType.MESH
        )
    pl.semaphore_wait(barrier, 2)

    def block(array, owner, way):
        rows = shards[array].shape[0]
        part = rows // 2
        start = pl.multiple_of(owner * rows + way * part, part)
        return wholes[array].at[pl.ds(start, part)]

    def hop(array, step, way):
        owner = device_at(place - step) if way == 0 else device_at(place + step)
        part = shards[array].shape[0] // 2
        target = block(array, owner, way)
        source = shards[array].at[pl.ds(way * part, part)] if step == 0 else target
        return pltpu.make_async_remote_copy(
            src_ref=source,
            dst_ref=target,
            send_sem=send_sem.at[way, step, array],
            recv_sem=recv_sem.at[way, step, array],
            device_id={"sp": ahead if way == 0 else behind},
            device_id_type=pl.DeviceIdType.MESH,
        )

    def arrival(array, step, way):
        owner = device_at(place - step - 1) if way == 0 else device_at(place + step + 1)
        target = block(array, owner, way)
        return pltpu.make_async_remote_copy(
            src_ref=target,
            dst_ref=target,
            send_sem=send_sem.at[way, step, array],
            recv_sem=recv_sem.at[way, step, array],
            device_id={"sp": ahead if way == 0 else behind},
            device_id_type=pl.DeviceIdType.MESH,
        )

    for array in range(count):
        for way in range(2):
            hop(array, 0, way).start()
    loads = [
        pltpu.make_async_copy(shards[a], bounce[a], in_sem.at[a]) for a in range(count)
    ]
    for load in loads:
        load.start()
    stores = []
    for a in range(count):
        loads[a].wait()
        rows = shards[a].shape[0]
        mine = wholes[a].at[pl.ds(pl.multiple_of(me * rows, rows), rows)]
        stores.append(pltpu.make_async_copy(bounce[a], mine, out_sem.at[a]))
        stores[a].start()
    for step in range(1, n - 1):
        for array in range(count):
            for way in range(2):
                arrival(array, step - 1, way).wait_recv()
                hop(array, step, way).start()
    for array in range(count):
        for way in range(2):
            arrival(array, n - 2, way).wait_recv()
    for step in range(n - 1):
        for array in range(count):
            for way in range(2):
                hop(array, step, way).wait_send()
    for store in stores:
        store.wait()


def ring_gather(arrays, collective_id):
    n = lax.axis_size("sp")
    count = len(arrays)
    return pl.pallas_call(
        functools.partial(ring_gather_kernel, n, count),
        out_shape=[
            jax.ShapeDtypeStruct((n * a.shape[0],) + a.shape[1:], a.dtype) for a in arrays
        ],
        in_specs=[pl.BlockSpec(memory_space=pl.ANY)] * count,
        out_specs=[pl.BlockSpec(memory_space=pl.ANY)] * count,
        scratch_shapes=[pltpu.VMEM(a.shape, a.dtype) for a in arrays]
        + [
            pltpu.SemaphoreType.DMA((count,)),
            pltpu.SemaphoreType.DMA((count,)),
            pltpu.SemaphoreType.DMA((2, n - 1, count)),
            pltpu.SemaphoreType.DMA((2, n - 1, count)),
        ],
        compiler_params=pltpu.CompilerParams(
            collective_id=collective_id, has_side_effects=True
        ),
    )(*arrays)


def per_device(
    tokens,
    norm_gain,
    w_query,
    w_key,
    w_value,
    w_glu,
    w_gate,
    sink_logit,
    conv_taps,
    conv_gain,
    out_attn,
    out_conv,
):
    row_count = tokens.shape[0]
    offset_rows = lax.axis_index("sp") * row_count
    positions = offset_rows + jnp.arange(row_count, dtype=jnp.int32)
    tokens_f = tokens.astype(jnp.float32)
    normed = (
        tokens_f
        * lax.rsqrt(jnp.mean(tokens_f * tokens_f, axis=1, keepdims=True) + 1e-06)
        * norm_gain
    ).astype(jnp.bfloat16)
    local_heads = w_query.shape[1] // HEAD
    local_kv = w_key.shape[1] // HEAD
    group_size = HEADS // KV
    kv_width = local_kv * HEAD
    *pieces, attn_rows, conv_rows = ring_gather(
        (w_query, w_key, w_value, w_glu, w_gate, out_attn, out_conv), 0
    )
    query_acc, key_acc, value_acc, glu_acc, gate_acc = tuple(
        (
            jnp.dot(normed, weight_piece, preferred_element_type=jnp.float32)
            for weight_piece in pieces
        )
    )
    queries = rotate_heads(query_acc.reshape(row_count, local_heads, HEAD), positions).astype(
        jnp.bfloat16
    )
    keys_rot = rotate_heads(key_acc.reshape(row_count, local_kv, HEAD), positions).astype(
        jnp.bfloat16
    )
    keys_rot = keys_rot.reshape(row_count, kv_width)
    values_bf = value_acc.astype(jnp.bfloat16)
    kv_tail = jnp.concatenate(
        [keys_rot[row_count - WINDOW :], values_bf[row_count - WINDOW :]], axis=1
    )
    kv_rim = passed_along(kv_tail, "sp", 1)
    gated = (glu_acc * jax.nn.sigmoid(gate_acc)).astype(jnp.bfloat16)
    conv_tail = gated[row_count - (KSIZE - 1) :]
    conv_rim = passed_along(conv_tail, "sp", 1)
    block_count = row_count // WINDOW
    keys_all = jnp.concatenate([kv_rim[:, :kv_width], keys_rot], axis=0).reshape(
        block_count + 1, WINDOW, local_kv, HEAD
    )
    vals_all = jnp.concatenate([kv_rim[:, kv_width:], values_bf], axis=0).reshape(
        block_count + 1, WINDOW, local_kv, HEAD
    )
    key_blocks = jnp.concatenate([keys_all[:-1], keys_all[1:]], axis=1)
    value_blocks = jnp.concatenate([vals_all[:-1], vals_all[1:]], axis=1)
    query_block_rows = queries.reshape(block_count, WINDOW, local_kv, group_size, HEAD)
    score_matrix = jnp.einsum(
        "bqhgd,bkhd->bhgqk", query_block_rows, key_blocks, preferred_element_type=jnp.float32
    ) * (1.0 / math.sqrt(HEAD))
    block_ids = jnp.arange(block_count, dtype=jnp.int32)[:, None, None]
    query_pos = (
        offset_rows + block_ids * WINDOW + jnp.arange(WINDOW, dtype=jnp.int32)[None, :, None]
    )
    key_pos = (
        offset_rows
        + (block_ids - 1) * WINDOW
        + jnp.arange(2 * WINDOW, dtype=jnp.int32)[None, None, :]
    )
    distance = query_pos - key_pos
    allowed = (distance >= 0) & (distance < WINDOW) & (key_pos >= 0)
    score_matrix = jnp.where(allowed[:, None, None], score_matrix, -1e30)
    sink_local = sink_logit.reshape(local_kv, group_size)[None, :, :, None, None]
    highest = jnp.maximum(jnp.max(score_matrix, axis=-1, keepdims=True), sink_local)
    weights_exp = jnp.exp(score_matrix - highest)
    denom_total = jnp.sum(weights_exp, axis=-1, keepdims=True) + jnp.exp(sink_local - highest)
    weights_bfloat_half = (weights_exp / denom_total).astype(jnp.bfloat16)
    attended_values = jnp.einsum(
        "bhgqk,bkhd->bqhgd", weights_bfloat_half, value_blocks, preferred_element_type=jnp.float32
    ).astype(jnp.bfloat16)
    attended_values = attended_values.reshape(row_count, local_heads * HEAD)
    extended = jnp.concatenate([conv_rim, gated], axis=0).astype(jnp.float32)
    filtered = lax.conv_general_dilated(
        extended[None],
        conv_taps.astype(jnp.float32)[:, None, :],
        (1,),
        "VALID",
        dimension_numbers=("NWC", "WIO", "NWC"),
        feature_group_count=extended.shape[1],
        precision=lax.Precision.HIGHEST,
    )[0]
    channel_sum, channel_square = lax.psum(
        (jnp.sum(filtered, axis=1), jnp.sum(filtered * filtered, axis=1)), "tp"
    )
    mean_value = channel_sum / CONV
    variance = channel_square / CONV - mean_value * mean_value
    scaled = (filtered - mean_value[:, None]) * lax.rsqrt(variance + 1e-05)[:, None] * conv_gain
    conv_out = jax.nn.silu(scaled).astype(jnp.bfloat16)
    pieces = (
        lax.all_gather(attended_values, "tp", axis=1, tiled=True),
        lax.all_gather(conv_out, "tp", axis=1, tiled=True),
    )
    mixed = jnp.dot(pieces[0], attn_rows, preferred_element_type=jnp.float32) + jnp.dot(
        pieces[1], conv_rows, preferred_element_type=jnp.float32
    )
    return mixed.astype(jnp.bfloat16)


def solution(mesh):
    return jax.shard_map(
        per_device,
        mesh=mesh,
        in_specs=(
            P("sp", None),
            P(),
            P("sp", "tp"),
            P("sp", "tp"),
            P("sp", "tp"),
            P("sp", "tp"),
            P("sp", "tp"),
            P("tp"),
            P(None, "tp"),
            P("tp"),
            P("sp", "tp"),
            P("sp", "tp"),
        ),
        out_specs=P("sp", "tp"),
        check_vma=False,
    )
```
